1024 devices in a mesh: sp: 16 (over z), dp: 64 (over y, x, core).
Axes of the slice: x: 4, y: 8, z: 16, core: 2. Of those that a mesh axis runs over, the one named last changes fastest.
Arguments:
- query_rows: bfloat16 [64, 2048, 1024], P('dp', 'sp'), may hold values from -5.5 to 5.5
- key_rows: bfloat16 [64, 2048, 1024], P('dp', 'sp'), may hold values from -5.5 to 5.5
- value_rows: bfloat16 [64, 2048, 1024], P('dp', 'sp'), may hold values from -6 to 6
- lambdas: float32 [8], replicated, may hold values from 0.3 to 0.8
- query_gain: float32 [64], replicated, may hold values from 1.1 to 8
- key_gain: float32 [64], replicated, may hold values from 1.1 to 8
- sub_gain: float32 [128], replicated, may hold values from 0.1 to 1.9
- out_weight: bfloat16 [1024, 2048], P(None, 'dp'), may hold values from -0.1875 to 0.1875
Outputs:
- attended: bfloat16 [64, 2048, 2048], P('dp', 'sp')
The draws below stay inside these ranges and needn't reach their ends.
All inputs are finite; a program needn't handle non-finite values.
Results may differ from the reference program's by a relative error of at most 0.0025.
The reference program's roundings to bfloat16 on the way count: a program that leaves them out, or rounds other values in their place, can miss the bound.
Values may be sent and summed in bfloat16 or wider, within the bound.
No kernel may reach another device: no remote copies, remote signals or barrier semaphores. Data moves between devices by JAX's collectives and lax.ppermute only.
A program may use at most 32 MiB of HBM per device.

```python
import jax
import jax.numpy as jnp
from jax import lax

D = 2048
HEADS = 8
HK = 64
HV = 128
LENGTH = 2048
SEQS = 64


def key_field(key):
    full_shape = (SEQS, LENGTH, 2 * HEADS * HK)
    key_base = jnp.clip(jax.random.normal(jax.random.fold_in(key, 101), full_shape, jnp.float32), -5.0, 5.0)
    return key_base


def draw_key_rows(key, part):
    return key_field(key).astype(jnp.bfloat16)


def draw_query_rows(key, part):
    full_shape = (SEQS, LENGTH, 2 * HEADS * HK)
    drawn_rows = jnp.clip(jax.random.normal(jax.random.fold_in(key, 107), full_shape, jnp.float32), -5.0, 5.0)
    return drawn_rows.astype(jnp.bfloat16)


def draw_query_gain(key, part):
    uniform_draw = jax.random.uniform(jax.random.fold_in(key, 211), (HK,), jnp.float32)
    return 1.1 + 0.5 * uniform_draw


def draw_key_gain(key, part):
    uniform_draw = jax.random.uniform(jax.random.fold_in(key, 223), (HK,), jnp.float32)
    return 1.1 + 0.5 * uniform_draw


def block_scale(own_key, shape, split, least, top_value):
    gain, own = 1.0, jax.random.fold_in(own_key, 6)
    for dim, shards_of in split:
        steps = jnp.exp(jax.random.uniform(jax.random.fold_in(own, dim), (shards_of,), jnp.float32, least / len(split), top_value / len(split)))
        gain = gain * jnp.repeat(steps, shape[dim] // shards_of).reshape([-1 if axis == dim else 1 for axis in range(len(shape))])
    return gain


def bell_draw(own_key, dims, scale, most, shards=(), kind=jnp.bfloat16):
    array = scale * jax.random.normal(own_key, dims, jnp.float32)
    if shards:
        array = array * block_scale(own_key, dims, shards, -0.22, 0.18)
    return jnp.clip(array, -most, most).astype(kind)


def setup_inputs(seed: int = 0) -> dict:
    keys = jax.random.split(jax.random.key(seed), 9)
    return {
        "query_rows": draw_query_rows(jax.random.fold_in(keys[8], 71), 0),
        "key_rows": draw_key_rows(jax.random.fold_in(keys[8], 71), 0),
        "value_rows": bell_draw(keys[2], (SEQS, LENGTH, HEADS * HV), 1.0, 6.0, ((0, 64), (1, 16))),
        "lambdas": jnp.clip(jax.random.uniform(keys[3], (HEADS,), jnp.float32, 0.3, 0.8), 0.3, 0.8),
        "query_gain": draw_query_gain(jax.random.fold_in(keys[8], 71), 0),
        "key_gain": draw_key_gain(jax.random.fold_in(keys[8], 71), 0),
        "sub_gain": jnp.clip(1.0 + 0.18 * jax.random.normal(keys[6], (HV,), jnp.float32), 0.1, 1.9),
        "out_weight": bell_draw(keys[7], (HEADS * HV, D), (HEADS * HV) ** -0.5, 0.1875, ((1, 64),)),
    }


epsilon = 1e-06
output_scale = 0.8

def normalize(field, scaling):
    return field * lax.rsqrt(lax.optimization_barrier(jnp.mean(field * field, axis=-1, keepdims=True)) + epsilon) * scaling

def reference(query_rows, key_rows, value_rows, lambdas, query_gain, key_gain, sub_gain, out_weight):
    sequences = query_rows.shape[0]
    length = query_rows.shape[1]
    groups = 2 * HEADS
    query_norm = normalize(query_rows.reshape(sequences, length, groups, HK).astype(jnp.float32), query_gain).astype(jnp.bfloat16)
    key_norm = normalize(key_rows.reshape(sequences, length, groups, HK).astype(jnp.float32), key_gain).astype(jnp.bfloat16)
    value_heads = value_rows.reshape(sequences, length, HEADS, HV)
    value_groups = jnp.concatenate([value_heads, value_heads], axis=2)
    positions = jnp.arange(length)
    causal = positions[None, :] <= positions[:, None]

    def one_group(inputs):
        group_query, group_key, group_value = inputs
        scores = jnp.dot(group_query, group_key.T, preferred_element_type=jnp.float32) * HK ** (-0.5)
        scores = jnp.where(causal, scores, -jnp.inf)
        weights = jax.nn.softmax(scores, axis=-1).astype(jnp.bfloat16)
        return jnp.dot(weights, group_value, preferred_element_type=jnp.float32).astype(jnp.bfloat16)

    def by_group(field):
        return jnp.transpose(field, (0, 2, 1, 3)).reshape(sequences * groups, length, field.shape[3])
    map_outputs = lax.map(one_group, (by_group(query_norm), by_group(key_norm), by_group(value_groups)))
    map_outputs = jnp.transpose(map_outputs.reshape(sequences, groups, length, HV), (0, 2, 1, 3)).astype(jnp.float32)
    mixed_heads = map_outputs[:, :, :HEADS] - lambdas[:, None] * map_outputs[:, :, HEADS:]
    normed = (normalize(mixed_heads, sub_gain) * output_scale).astype(jnp.bfloat16).reshape(sequences * length, HEADS * HV)
    projected = jnp.dot(normed, out_weight, preferred_element_type=jnp.float32)
    return projected.astype(jnp.bfloat16).reshape(sequences, length, D)
```

```python
import jax
import jax.numpy as jnp
from jax import lax
from jax.experimental import pallas as pl
from jax.experimental.pallas import tpu as pltpu
from jax.sharding import Mesh, PartitionSpec as P

HEADS = 8
HK = 64
HV = 128
EPS = 1e-06
OUT_SCALE = 0.8
F32 = jnp.float32
BF16 = jnp.bfloat16
SWAP = [(0, 1), (1, 0)]


def limit(mib):
    return pltpu.CompilerParams(vmem_limit_bytes=mib * 1024 * 1024)


def anywhere():
    return pl.BlockSpec(memory_space=pl.ANY)


def vmem():
    return pl.BlockSpec(memory_space=pltpu.VMEM)


def smem():
    return pl.BlockSpec(memory_space=pltpu.SMEM)


def slice_kernel(q_ref, k_ref, v_ref, out_ref, sems):
    half = out_ref.shape[0]
    start = pl.multiple_of((1 - lax.axis_index("core")) * half, half)
    width = q_ref.shape[2]
    copies = [
        pltpu.make_async_copy(
            ref.at[0, pl.ds(start, half), :], out_ref.at[:, pl.ds(n * width, width)], sems.at[n]
        )
        for n, ref in enumerate((q_ref, k_ref, v_ref))
    ]
    for copy in copies:
        copy.start()
    for copy in copies:
        copy.wait()


def pack_kernel(q_ref, k_ref, v_ref, recv_ref, qg_ref, kg_ref, out_ref, gain_ref):
    core = lax.axis_index("core")
    half = recv_ref.shape[0]
    width = HEADS * HV
    lane = lax.broadcasted_iota(jnp.int32, (half, 128), 1)
    low = lane < HK
    block = (
        lax.broadcasted_iota(jnp.int32, (128, 128), 0) // HK
        == lax.broadcasted_iota(jnp.int32, (128, 128), 1) // HK
    ).astype(F32).astype(BF16)

    def norm(tile, gain):
        x = tile.astype(F32)
        square = x * x
        high = square.astype(BF16)
        rest = (square - high.astype(F32)).astype(BF16)
        total = jnp.dot(high, block, preferred_element_type=F32) + jnp.dot(
            rest, block, preferred_element_type=F32
        )
        return x * lax.rsqrt(total * (1.0 / HK) + EPS) * gain

    def side(read, base):
        for name, offset in ((0, 0), (1, 128)):
            gain = gain_ref[name : name + 1, :]
            for pair in range(HEADS // 2):
                first = norm(read(name, pair * 128), gain)
                second = norm(read(name, (pair + HEADS // 2) * 128), gain)
                even = jnp.where(low, first, pltpu.roll(second, HK, 1))
                odd = jnp.where(low, pltpu.roll(first, HK, 1), second)
                out_ref[base + 2 * pair, :, offset : offset + 128] = even.astype(BF16)
                out_ref[base + 2 * pair + 1, :, offset : offset + 128] = odd.astype(BF16)
        for head in range(HEADS):
            out_ref[base + head, :, 256:384] = read(2, head * 128)

    for n in range(2):
        gain_ref[0:1, n * HK : n * HK + HK] = qg_ref[...] * (HK ** -0.5)
        gain_ref[1:2, n * HK : n * HK + HK] = kg_ref[...]
    own = (q_ref, k_ref, v_ref)
    start = pl.multiple_of(core * half, half)
    side(lambda n, c: own[n][0, pl.ds(start, half), c : c + 128], core * HEADS)
    side(lambda n, c: recv_ref[:, n * width + c : n * width + c + 128], (1 - core) * HEADS)


def attend_kernel(own_ref, far_ref, lam_ref, sg_ref, out_ref, s_ref, p_ref, vt_ref):
    core = lax.axis_index("core")
    lam = lam_ref[lax.axis_index("sp") % HEADS]
    rows = own_ref.shape[0]
    tile = 256
    lane = lax.broadcasted_iota(jnp.int32, (tile, 128), 1)
    key_row = lax.broadcasted_iota(jnp.int32, (tile, tile), 0)
    query_row = lax.broadcasted_iota(jnp.int32, (tile, tile), 1)
    own_mask = key_row <= query_row
    far_mask = key_row // 64 < query_row // 64 + core
    for n in range(rows // 128):
        vt_ref[:, n * 128 : n * 128 + 128] = own_ref[n * 128 : n * 128 + 128, 256:384].T
        vt_ref[:, rows + n * 128 : rows + n * 128 + 128] = far_ref[n * 128 : n * 128 + 128, 128:256].T
    for t in range(rows // tile):
        q = own_ref[t * tile : t * tile + tile, 0:128]
        maps = []
        for m in range(2):
            qm = jnp.where((lane < HK) == (m == 0), q, jnp.zeros_like(q))
            top = jnp.full((8, tile), -jnp.inf, F32)
            for side in range(2):
                for n in range(t + 1):
                    if side == 0:
                        k = own_ref[n * tile : n * tile + tile, 128:256]
                    else:
                        k = far_ref[n * tile : n * tile + tile, 0:128]
                    s = lax.dot_general(k, qm, (((1,), (1,)), ((), ())), preferred_element_type=F32)
                    if n == t:
                        s = jnp.where(own_mask if side == 0 else far_mask, s, -jnp.inf)
                    at = (side * (t + 1) + n) * tile
                    s_ref[at : at + tile, :] = s
                    top = jnp.maximum(top, jnp.max(s.reshape(tile // 8, 8, tile), axis=0))
            peak = jnp.max(top, axis=0, keepdims=True)
            total = jnp.zeros((8, tile), F32)
            count = 2 * (t + 1)
            for n in range(count):
                e = jnp.exp(s_ref[n * tile : n * tile + tile, :] - peak)
                total = total + jnp.sum(e.reshape(tile // 8, 8, tile), axis=0)
                s_ref[n * tile : n * tile + tile, :] = e
            inverse = 1.0 / jnp.sum(total, axis=0, keepdims=True)
            for n in range(count):
                p_ref[n * tile : n * tile + tile, :] = (
                    s_ref[n * tile : n * tile + tile, :] * inverse
                ).astype(BF16)
            span = (t + 1) * tile
            o = jnp.dot(vt_ref[:, :span], p_ref[:span, :], preferred_element_type=F32) + jnp.dot(
                vt_ref[:, rows : rows + span], p_ref[span : 2 * span, :], preferred_element_type=F32
            )
            maps.append(o.astype(BF16).astype(F32))
        mixed = maps[0] - lam * maps[1]
        mean = jnp.sum(mixed * mixed, axis=0, keepdims=True) * (1.0 / HV)
        scaled = (mixed * lax.rsqrt(mean + EPS)).T
        out_ref[t * tile : t * tile + tile, :] = (scaled * sg_ref[...] * OUT_SCALE).astype(BF16)


def project_kernel(got_ref, far_ref, *refs):
    *w_refs, out_ref, x_ref, xt_ref, wide_ref = refs
    core = lax.axis_index("core")
    half = far_ref.shape[1]
    tokens = 2 * half
    own_at = pl.multiple_of(core * half, half)
    far_at = pl.multiple_of((1 - core) * half, half)
    for h in range(HEADS):
        x_ref[pl.ds(own_at, half), h * HV : h * HV + HV] = got_ref[core * HEADS + h]
        x_ref[pl.ds(far_at, half), h * HV : h * HV + HV] = far_ref[h]
    for h in range(HEADS):
        xt_ref[h * HV : h * HV + HV, :] = x_ref[:, h * HV : h * HV + HV].T
    xs = lax.axis_size("x")
    mine = lax.axis_index("x")
    rows = w_refs[0].shape[0]
    ys = lax.axis_size("y")
    cols = rows // ys
    xt = xt_ref[...]
    for n, ref in enumerate(w_refs):
        shift = (0, xs - 1, 1, 2)[n % (len(w_refs) // 2)]
        side = core if n < len(w_refs) // 2 else 1 - core
        base = lax.rem(mine + shift, xs) * (2 * cols) + side * cols
        block = jnp.dot(ref[...], xt, preferred_element_type=F32)
        for y in range(ys):
            wide_ref[pl.ds(pl.multiple_of(base + y * (2 * xs * cols), cols), cols), :] = block[
                y * cols : y * cols + cols
            ]
    total = wide_ref.shape[0]
    for n in range(0, total, 128):
        span = min(128, total - n)
        out_ref[0, :, n : n + span] = wide_ref[n : n + span, :].T.astype(BF16)


def gather_weight(out_weight):
    xs = lax.axis_size("x")
    mine = lax.all_gather(out_weight.T, "y", axis=0, tiled=True)
    if xs == 1:
        return [mine]
    up = [(i, (i + 1) % xs) for i in range(xs)]
    down = [(i, (i - 1) % xs) for i in range(xs)]
    left = lax.ppermute(mine, "x", up)
    right = lax.ppermute(mine, "x", down)
    cut = mine.shape[0] // 2
    first = lax.ppermute(left[:cut], "x", up)
    second = lax.ppermute(right[cut:], "x", down)
    return [mine, left, right, jnp.concatenate([first, second], axis=0)]


def body(query_rows, key_rows, value_rows, lambdas, query_gain, key_gain, sub_gain, out_weight):
    core = lax.axis_index("core")
    sp = lax.axis_size("sp")
    tokens = query_rows.shape[1]
    half = tokens // 2
    width = HEADS * HV

    outgoing = pl.pallas_call(
        slice_kernel,
        out_shape=jax.ShapeDtypeStruct((half, 3 * width), BF16),
        in_specs=[anywhere()] * 3,
        out_specs=anywhere(),
        scratch_shapes=[pltpu.SemaphoreType.DMA((3,))],
        compiler_params=limit(4),
        name="slice",
    )(query_rows, key_rows, value_rows)
    received = lax.ppermute(outgoing, "core", SWAP)
    packet = pl.pallas_call(
        pack_kernel,
        out_shape=jax.ShapeDtypeStruct((sp, half, 384), BF16),
        in_specs=[vmem()] * 6,
        out_specs=vmem(),
        scratch_shapes=[pltpu.VMEM((2, 128), F32)],
        compiler_params=limit(8),
        name="pack",
    )(query_rows, key_rows, value_rows, received, query_gain[None], key_gain[None])
    packet, out_weight = lax.optimization_barrier((packet, out_weight))
    weights = gather_weight(out_weight)
    arrived = lax.all_to_all(packet, "sp", split_axis=0, concat_axis=0, tiled=True).reshape(sp * half, 384)
    arrived, weights = lax.optimization_barrier((arrived, weights))
    far = lax.ppermute(arrived[:, 128:384], "core", SWAP)
    rows = sp * half
    normed = pl.pallas_call(
        attend_kernel,
        out_shape=jax.ShapeDtypeStruct((rows, HV), BF16),
        in_specs=[vmem(), vmem(), smem(), vmem()],
        out_specs=vmem(),
        scratch_shapes=[
            pltpu.VMEM((2 * rows, 256), F32),
            pltpu.VMEM((2 * rows, 256), BF16),
            pltpu.VMEM((HV, 2 * rows), BF16),
        ],
        compiler_params=limit(24),
        name="attend",
    )(arrived, far, lambdas, sub_gain[None])
    normed, weights = lax.optimization_barrier((normed, weights))
    weights = weights + [lax.ppermute(part, "core", SWAP) for part in weights]
    got = lax.all_to_all(normed.reshape(sp, half, HV), "sp", split_axis=0, concat_axis=0, tiled=True)
    got, weights = lax.optimization_barrier((got, weights))
    got_far = lax.ppermute(
        lax.dynamic_slice_in_dim(got, (1 - core) * HEADS, HEADS, axis=0), "core", SWAP
    )
    columns = 2 * len(weights) // 2 * weights[0].shape[0]
    return pl.pallas_call(
        project_kernel,
        out_shape=jax.ShapeDtypeStruct((1, tokens, columns), BF16),
        in_specs=[vmem()] * (2 + len(weights)),
        out_specs=vmem(),
        scratch_shapes=[
            pltpu.VMEM((tokens, width), BF16),
            pltpu.VMEM((width, tokens), BF16),
            pltpu.VMEM((columns, tokens), F32),
        ],
        compiler_params=limit(16),
        name="project",
    )(got, got_far, *weights)


def solution(mesh):
    sp, dp = mesh.devices.shape
    xs = 4 if dp >= 8 else 1
    fine = Mesh(mesh.devices.reshape(sp, dp // (2 * xs), xs, 2), ("sp", "y", "x", "core"))
    rows = P(("y", "x", "core"), "sp", None)
    in_specs = (rows, rows, rows, P(), P(), P(), P(), P(None, ("y", "x", "core")))
    return jax.shard_map(body, mesh=fine, in_specs=in_specs, out_specs=rows, check_vma=False)
```
